32 devices in a mesh: sp: 8 (over z, y), tp: 4 (over x, core).
Axes of the slice: x: 2, y: 2, z: 4, core: 2. Of those that a mesh axis runs over, the one named last changes fastest.
Arguments:
- tokens: bfloat16 [2048, 4096], P('sp', 'tp'), may hold values from -6 to 6
- input_norm_gain: float32 [4096], replicated, may hold values from 0.1 to 1.9
- query_weight: bfloat16 [4096, 2048], P('sp', 'tp'), may hold values from -0.09375 to 0.09375
- key_weight: bfloat16 [4096, 2048], P('sp', 'tp'), may hold values from -0.09375 to 0.09375
- value_weight: bfloat16 [4096, 2048], P('sp', 'tp'), may hold values from -0.09375 to 0.09375
- decay_first_map: bfloat16 [4096, 128], replicated, may hold values from -0.09375 to 0.09375
- decay_second_map: bfloat16 [128, 2048], P(None, 'tp'), may hold values from -0.5 to 0.5
- channel_decay_offset: float32 [2048], P('tp'), may hold values from -13 to -2
- position_decay_offset: float32 [2048], P('sp'), may hold values from -2 to 2
- extra_log_decay: float32 [2048, 32], P('sp', 'tp'), may hold values from -0.7 to 0
- rate_first_map: bfloat16 [4096, 128], replicated, may hold values from -0.09375 to 0.09375
- rate_second_map: bfloat16 [128, 2048], P(None, 'tp'), may hold values from -0.25 to 0.25
- channel_rate_offset: float32 [2048], P('tp'), may hold values from -10 to 1
- own_term_weight: float32 [2048], P('tp'), may hold values from -2 to 2
- head_norm_gain: float32 [2048], P('tp'), may hold values from 0.1 to 1.9
- starting_state: float32 [32, 64, 64], P('tp'), may hold values from -192 to 192
- outer_gate_weight: bfloat16 [4096, 2048], P('sp', 'tp'), may hold values from -0.09375 to 0.09375
- inner_gate_weight: bfloat16 [4096, 2048], P('sp', 'tp'), may hold values from -0.09375 to 0.09375
- signal_weight: bfloat16 [4096, 2048], P('sp', 'tp'), may hold values from -0.09375 to 0.09375
- convolution_taps: bfloat16 [3, 2048], P(None, 'tp'), may hold values from -3.5 to 3.5
- convolution_gain: float32 [2048], P('tp'), may hold values from 0.1 to 1.9
Outputs:
- linear_attention_output: bfloat16 [2048, 2048], P('sp', 'tp')
- out_conv: bfloat16 [2048, 2048], P('sp', 'tp')
The draws below stay inside these ranges and needn't reach their ends.
All inputs are finite; a program needn't handle non-finite values.
Results may differ from the reference program's by a relative error of at most 0.009.
Values may be sent and summed in bfloat16 or wider, within the bound.
A program may use at most 128 MiB of HBM per device.

```python
import math
import jax
import jax.numpy as jnp
from jax import lax

D = 4096
HEAD_COUNT = 32
HEAD_SIZE = 64
RANK = 128
TAPS = 3
BLOCK = 64
TOK_DEV = 256
MIXER_WIDTH = 2048
TOKEN_COUNT = 2048


def pick_slow(key):
    ranking = jax.random.permutation(jax.random.fold_in(key, 7), HEAD_COUNT)
    slow_count = HEAD_COUNT // 2
    return jnp.repeat(ranking < slow_count, HEAD_SIZE)


def draw_channel_decay_offset(key, part):
    slow_mask = pick_slow(key)
    jitter = jax.random.uniform(jax.random.fold_in(key, 21), (HEAD_COUNT * HEAD_SIZE,), jnp.float32, -0.5, 0.5)
    fast_values = jax.random.uniform(jax.random.fold_in(key, 22), (HEAD_COUNT * HEAD_SIZE,), jnp.float32, -3.5, -2.5)
    return jnp.where(slow_mask, -math.log(TOKEN_COUNT) - 1.0 + jitter, fast_values)


def draw_channel_rate_offset(key, part):
    slow_mask = pick_slow(key)
    jitter = jax.random.uniform(jax.random.fold_in(key, 23), (HEAD_COUNT * HEAD_SIZE,), jnp.float32, -0.5, 0.5)
    fast_values = jax.random.uniform(jax.random.fold_in(key, 24), (HEAD_COUNT * HEAD_SIZE,), jnp.float32, -1.0, 1.0)
    return jnp.where(slow_mask, math.log(8.0 / TOKEN_COUNT) + jitter, fast_values)


def draw_position_decay_offset(key, part):
    positions = jnp.arange(TOKEN_COUNT)
    per_block = jax.random.uniform(jax.random.fold_in(key, 31), (TOKEN_COUNT // BLOCK,), jnp.float32, -1.0, 1.0)
    per_device = jax.random.uniform(jax.random.fold_in(key, 32), (TOKEN_COUNT // TOK_DEV,), jnp.float32, -0.7, 0.7)
    return per_block[positions // BLOCK] + per_device[positions // TOK_DEV]


def draw_extra_log_decay(key, part):
    spots = jax.random.permutation(jax.random.fold_in(key, 41), TOKEN_COUNT)[:3]
    losses = jnp.log(jax.random.uniform(jax.random.fold_in(key, 42), (3, HEAD_COUNT), jnp.float32, 0.5, 0.8))
    markers = (jnp.arange(TOKEN_COUNT)[:, None] == spots[None, :]).astype(jnp.float32)
    return jnp.dot(markers, losses)


def draw_starting_state(key, part):
    spread = math.sqrt(TOKEN_COUNT)
    values = jnp.clip(jax.random.normal(jax.random.fold_in(key, 52), (HEAD_COUNT, HEAD_SIZE, HEAD_SIZE), jnp.float32), -6.0, 6.0) * 0.7
    return values * spread


def block_scale(own_key, extent, shards, least, high):
    factor_of, own = 1.0, jax.random.fold_in(own_key, 6)
    for position, shards_of in shards:
        draws = jnp.exp(jax.random.uniform(jax.random.fold_in(own, position), (shards_of,), jnp.float32, least / len(shards), high / len(shards)))
        factor_of = factor_of * jnp.repeat(draws, extent[position] // shards_of).reshape([-1 if axis == position else 1 for axis in range(len(extent))])
    return factor_of


def normal_values(rng, dims, width, most, cuts=(), held_as=jnp.bfloat16):
    result = jax.random.normal(rng, dims, jnp.float32) * width
    if len(cuts) > 0:
        result = block_scale(rng, dims, cuts, -0.22, 0.18) * result
    return jnp.clip(result, min=-most, max=most).astype(held_as)


def setup_inputs(seed: int = 0) -> dict:
    key_list = jax.random.split(jax.random.key(seed), 22)
    tokens = normal_values(key_list[0], (TOKEN_COUNT, D), 1.0, 6.0, ((0, 8), (1, 4)))
    input_norm_gain = jnp.clip(1.0 + 0.18 * jax.random.normal(key_list[1], (D,), jnp.float32), 0.1, 1.9)
    query_weight = normal_values(key_list[2], (D, MIXER_WIDTH), D ** -0.5, 0.09375, ((0, 8), (1, 4)))
    key_weight = normal_values(key_list[3], (D, MIXER_WIDTH), D ** -0.5, 0.09375, ((0, 8), (1, 4)))
    value_weight = normal_values(key_list[4], (D, MIXER_WIDTH), D ** -0.5, 0.09375, ((0, 8), (1, 4)))
    decay_first_map = normal_values(key_list[5], (D, RANK), D ** -0.5, 0.09375)
    decay_second_map = normal_values(key_list[6], (RANK, MIXER_WIDTH), RANK ** -0.5, 0.5, ((1, 4),))
    channel_decay_offset = draw_channel_decay_offset(jax.random.fold_in(key_list[21], 71), 0)
    position_decay_offset = draw_position_decay_offset(jax.random.fold_in(key_list[21], 71), 0)
    extra_log_decay = draw_extra_log_decay(jax.random.fold_in(key_list[21], 71), 0)
    rate_first_map = normal_values(key_list[10], (D, RANK), D ** -0.5, 0.09375)
    rate_second_map = normal_values(key_list[11], (RANK, MIXER_WIDTH), (4 * RANK) ** -0.5, 0.25, ((1, 4),))
    channel_rate_offset = draw_channel_rate_offset(jax.random.fold_in(key_list[21], 71), 0)
    own_term_weight = normal_values(key_list[13], (MIXER_WIDTH,), 0.125, 2.0, ((0, 4),), jnp.float32)
    head_norm_gain = jnp.clip(1.0 + 0.18 * jax.random.normal(key_list[14], (MIXER_WIDTH,), jnp.float32), 0.1, 1.9)
    starting_state = draw_starting_state(jax.random.fold_in(key_list[21], 71), 0)
    outer_gate_weight = normal_values(key_list[16], (D, MIXER_WIDTH), D ** -0.5, 0.09375, ((0, 8), (1, 4)))
    inner_gate_weight = normal_values(key_list[17], (D, MIXER_WIDTH), D ** -0.5, 0.09375, ((0, 8), (1, 4)))
    signal_weight = normal_values(key_list[18], (D, MIXER_WIDTH), D ** -0.5, 0.09375, ((0, 8), (1, 4)))
    convolution_taps = normal_values(key_list[19], (TAPS, MIXER_WIDTH), TAPS ** -0.5, 3.5, ((1, 4),))
    convolution_gain = jnp.clip(1.0 + 0.18 * jax.random.normal(key_list[20], (MIXER_WIDTH,), jnp.float32), 0.1, 1.9)
    return {"tokens": tokens, "input_norm_gain": input_norm_gain, "query_weight": query_weight, "key_weight": key_weight, "value_weight": value_weight, "decay_first_map": decay_first_map, "decay_second_map": decay_second_map, "channel_decay_offset": channel_decay_offset, "position_decay_offset": position_decay_offset, "extra_log_decay": extra_log_decay, "rate_first_map": rate_first_map, "rate_second_map": rate_second_map, "channel_rate_offset": channel_rate_offset, "own_term_weight": own_term_weight, "head_norm_gain": head_norm_gain, "starting_state": starting_state, "outer_gate_weight": outer_gate_weight, "inner_gate_weight": inner_gate_weight, "signal_weight": signal_weight, "convolution_taps": convolution_taps, "convolution_gain": convolution_gain}


DECAY_FACTOR = 0.606531
NORM_EPS = 1e-06
GROUP_EPS = 0.00064
KEY_EPS = 1e-06

def rounded(values):
    return lax.optimization_barrier(values.astype(jnp.bfloat16)).astype(jnp.float32)

def project(normed, weight):
    return rounded(jnp.dot(normed, weight, preferred_element_type=jnp.float32))

def recurrence(state, inputs):
    query, decay, keyed, valued, unit_key, rate = inputs
    removal = jnp.einsum('hvk,hk->hv', state, -unit_key, precision=lax.Precision.HIGHEST)
    state = state * decay[:, None, :] + removal[:, :, None] * (unit_key * rate)[:, None, :] + valued[:, :, None] * keyed[:, None, :]
    recalled = jnp.einsum('hvk,hk->hv', state, query, precision=lax.Precision.HIGHEST)
    return (state, recalled)

def reference(tokens, input_norm_gain, query_weight, key_weight, value_weight, decay_first_map, decay_second_map, channel_decay_offset, position_decay_offset, extra_log_decay, rate_first_map, rate_second_map, channel_rate_offset, own_term_weight, head_norm_gain, starting_state, outer_gate_weight, inner_gate_weight, signal_weight, convolution_taps, convolution_gain):
    wide = tokens.astype(jnp.float32)
    normed = (wide * lax.rsqrt(lax.optimization_barrier(jnp.mean(wide * wide, axis=1, keepdims=True)) + NORM_EPS) * input_norm_gain.astype(jnp.float32)).astype(jnp.bfloat16)
    query = project(normed, query_weight)
    keyed = project(normed, key_weight)
    valued = project(normed, value_weight)
    decay_low = jnp.tanh(jnp.dot(normed, decay_first_map, preferred_element_type=jnp.float32)).astype(jnp.bfloat16)
    decay_logits = channel_decay_offset + jnp.dot(decay_low, decay_second_map, preferred_element_type=jnp.float32) + position_decay_offset[:, None]
    decay_logarithm = -DECAY_FACTOR * jax.nn.sigmoid(decay_logits) + jnp.repeat(extra_log_decay, HEAD_SIZE, axis=1)
    rate_low = jnp.dot(normed, rate_first_map, preferred_element_type=jnp.float32).astype(jnp.bfloat16)
    rate = jax.nn.sigmoid(channel_rate_offset + jnp.dot(rate_low, rate_second_map, preferred_element_type=jnp.float32))
    head_shape = (TOKEN_COUNT, HEAD_COUNT, HEAD_SIZE)
    query_per_head = query.reshape(head_shape)
    key_per_head = keyed.reshape(head_shape)
    value_per_head = valued.reshape(head_shape)
    unit_key = key_per_head * lax.rsqrt(lax.optimization_barrier(jnp.sum(key_per_head * key_per_head, axis=2, keepdims=True)) + KEY_EPS)
    inputs = (query_per_head, jnp.exp(decay_logarithm).reshape(head_shape), key_per_head, value_per_head, unit_key, rate.reshape(head_shape))
    final_state, recalled = lax.scan(recurrence, starting_state, inputs)
    center = recalled - lax.optimization_barrier(jnp.mean(recalled, axis=2, keepdims=True))
    variance = lax.optimization_barrier(jnp.mean(center * center, axis=2, keepdims=True))
    input_normed = center * lax.rsqrt(variance + GROUP_EPS) * head_norm_gain.reshape(HEAD_COUNT, HEAD_SIZE)
    own_term = lax.optimization_barrier(jnp.sum(query_per_head * key_per_head * own_term_weight.reshape(HEAD_COUNT, HEAD_SIZE), axis=2, keepdims=True)) * value_per_head
    linear_attention_output = (input_normed + own_term).reshape(TOKEN_COUNT, MIXER_WIDTH).astype(jnp.bfloat16)
    outer = project(normed, outer_gate_weight)
    inner = project(normed, inner_gate_weight)
    signal = project(normed, signal_weight)
    mixed_in = rounded(inner * signal)
    padded = jnp.concatenate([jnp.zeros((2, MIXER_WIDTH), jnp.float32), mixed_in], axis=0)
    taps = convolution_taps.astype(jnp.float32)
    gated = outer * (taps[0] * padded[:-2] + taps[1] * padded[1:-1] + taps[2] * padded[2:])
    out_conv = (gated * lax.rsqrt(lax.optimization_barrier(jnp.mean(gated * gated, axis=1, keepdims=True)) + NORM_EPS) * convolution_gain).astype(jnp.bfloat16)
    return (linear_attention_output, out_conv)
```

```python
import functools

import jax
import jax.numpy as jnp
from jax import lax
from jax.experimental import pallas as pl
from jax.experimental.pallas import tpu as pltpu
from jax.sharding import PartitionSpec as P

BLOCK = 64


DECAY_FACTOR = 0.606531
NORM_EPS = 1e-06
GROUP_EPS = 0.00064
KEY_EPS = 1e-06


def from_behind(block, axis, distance):
    devices = range(lax.axis_size(axis))
    route = [(i - distance, i) for i in devices if i - distance in devices]
    return lax.ppermute(block, axis, route)


def rounded(values):
    return lax.optimization_barrier(values.astype(jnp.bfloat16)).astype(jnp.float32)


def contract(spec, left, right):
    return jnp.einsum(spec, left, right, precision=lax.Precision.HIGHEST)


def fold_rows(normed):

    def accumulate(totals, pieces, offset):
        return tuple(
            (
                jnp.dot(normed, weight_piece, preferred_element_type=jnp.float32)
                for weight_piece in pieces
            )
        )

    return accumulate


def mixer_blocks(query, keyed, valued, unit_key, decay_logarithm, rate):
    sequence_length, number_heads, head_dimension = query.shape
    block_size = BLOCK
    count = sequence_length // block_size
    eye_heads = jnp.broadcast_to(
        jnp.eye(head_dimension, dtype=jnp.float32), (number_heads, head_dimension, head_dimension)
    )
    eye_block = jnp.eye(block_size, dtype=jnp.float32)
    later = jnp.arange(block_size)[:, None]
    earlier = jnp.arange(block_size)[None, :]
    strict = later > earlier
    inclusive = later >= earlier
    block_shape = (count, block_size, number_heads, head_dimension)
    query_b, keyed_b, valued_b, unit_b, decay_b, rate_b = (
        values.reshape(block_shape)
        for values in (query, keyed, valued, unit_key, decay_logarithm, rate)
    )
    cumul = jnp.cumsum(decay_b, axis=1)
    before = cumul - decay_b
    a_prime = -unit_b * jnp.exp(before)
    b_scaled = unit_b * rate_b * jnp.exp(-cumul)
    k_scaled = keyed_b * jnp.exp(-cumul)
    r_prime = query_b * jnp.exp(cumul)
    removal = jnp.where(strict, contract("cthn,cshn->chts", a_prime, b_scaled), 0.0)
    writes = jnp.where(strict, contract("cthn,cshn->chts", a_prime, k_scaled), 0.0)
    reads = jnp.where(inclusive, contract("cthn,cshn->chts", r_prime, b_scaled), 0.0)
    key_reads = jnp.where(inclusive, contract("cthn,cshn->chts", r_prime, k_scaled), 0.0)
    power = removal
    inverse = eye_block + removal
    reach = 2
    while reach < block_size:
        power = contract("chts,chsu->chtu", power, power)
        inverse = inverse + contract("chts,chsu->chtu", inverse, power)
        reach = reach * 2
    unit_solved = contract("chts,cshn->chtn", inverse, a_prime)
    free_solved = contract(
        "chts,chsv->chtv", inverse, contract("chts,cshv->chtv", writes, valued_b)
    )
    probe_raw = jnp.transpose(r_prime, (0, 2, 1, 3)) + contract(
        "chts,chsn->chtn", reads, unit_solved
    )
    free_read = contract("chts,chsv->chtv", reads, free_solved) + contract(
        "chts,cshv->chtv", key_reads, valued_b
    )
    closing = jnp.exp(cumul[:, -1])
    b_end = b_scaled * closing[:, None]
    k_end = k_scaled * closing[:, None]
    step_map = eye_heads[None] * closing[:, :, None, :] + contract(
        "chtj,cthk->chjk", unit_solved, b_end
    )
    constant = contract("chtv,cthk->chvk", free_solved, b_end) + contract(
        "cthv,cthk->chvk", valued_b, k_end
    )
    local_state = jnp.zeros((number_heads, head_dimension, head_dimension), jnp.float32)
    product = eye_heads
    entering_states = []
    entering_maps = []
    for index in range(count):
        entering_states.append(local_state)
        entering_maps.append(product)
        local_state = contract("hvk,hkj->hvj", local_state, step_map[index]) + constant[index]
        product = contract("hij,hjk->hik", product, step_map[index])
    stacked_states = jnp.stack(entering_states)
    stacked_maps = jnp.stack(entering_maps)
    recalled = contract("chvk,chtk->cthv", stacked_states, probe_raw) + jnp.transpose(
        free_read, (0, 2, 1, 3)
    )
    probe = contract("chjk,chtk->cthj", stacked_maps, probe_raw)
    head_shape = (sequence_length, number_heads, head_dimension)
    return (recalled.reshape(head_shape), probe.reshape(head_shape), local_state, product)


def mixer_local(
    normed,
    projected,
    decay_first_map,
    decay_second_map,
    channel_decay_offset,
    position_decay_offset,
    extra_log_decay,
    rate_first_map,
    rate_second_map,
    channel_rate_offset,
):
    query, keyed, valued = (rounded(values) for values in projected)
    sequence_length = normed.shape[0]
    number_heads = extra_log_decay.shape[1]
    head_dimension = query.shape[1] // number_heads
    decay_low = jnp.tanh(
        jnp.dot(normed, decay_first_map, preferred_element_type=jnp.float32)
    ).astype(jnp.bfloat16)
    decay_logits = (
        channel_decay_offset
        + jnp.dot(decay_low, decay_second_map, preferred_element_type=jnp.float32)
        + position_decay_offset[:, None]
    )
    decay_logarithm = -DECAY_FACTOR * jax.nn.sigmoid(decay_logits) + jnp.repeat(
        extra_log_decay, head_dimension, axis=1
    )
    rate_low = jnp.dot(normed, rate_first_map, preferred_element_type=jnp.float32).astype(
        jnp.bfloat16
    )
    rate = jax.nn.sigmoid(
        channel_rate_offset + jnp.dot(rate_low, rate_second_map, preferred_element_type=jnp.float32)
    )
    head_shape = (sequence_length, number_heads, head_dimension)
    query_per_head = query.reshape(head_shape)
    key_per_head = keyed.reshape(head_shape)
    value_per_head = valued.reshape(head_shape)
    unit_key = key_per_head * lax.rsqrt(
        jnp.sum(key_per_head * key_per_head, axis=2, keepdims=True) + KEY_EPS
    )
    recalled, probe, final_state, final_product = mixer_blocks(
        query_per_head,
        key_per_head,
        value_per_head,
        unit_key,
        decay_logarithm.reshape(head_shape),
        rate.reshape(head_shape),
    )
    return (
        (query_per_head, key_per_head, value_per_head),
        recalled,
        probe,
        final_state,
        final_product,
    )


def shards(
    tokens,
    input_norm_gain,
    query_weight,
    key_weight,
    value_weight,
    decay_first_map,
    decay_second_map,
    channel_decay_offset,
    position_decay_offset,
    extra_log_decay,
    rate_first_map,
    rate_second_map,
    channel_rate_offset,
    own_term_weight,
    head_norm_gain,
    starting_state,
    outer_gate_weight,
    inner_gate_weight,
    signal_weight,
    convolution_taps,
    convolution_gain,
):
    whole = lax.all_gather(tokens, "tp", axis=1, tiled=True)
    wide = whole.astype(jnp.float32)
    normed = (
        wide * lax.rsqrt(jnp.mean(wide * wide, axis=1, keepdims=True) + NORM_EPS) * input_norm_gain
    ).astype(jnp.bfloat16)
    sequence_length = normed.shape[0]
    accumulate = fold_rows(normed)
    empty = jnp.zeros((sequence_length, query_weight.shape[1]), jnp.float32)
    mixer_args = (
        decay_first_map,
        decay_second_map,
        channel_decay_offset,
        position_decay_offset,
        extra_log_decay,
        rate_first_map,
        rate_second_map,
        channel_rate_offset,
    )
    query, keyed, valued, outer, inner, signal = accumulate(
        (empty, empty, empty, empty, empty, empty),
        (
            lax.all_gather(query_weight, "sp", axis=0, tiled=True),
            lax.all_gather(key_weight, "sp", axis=0, tiled=True),
            lax.all_gather(value_weight, "sp", axis=0, tiled=True),
            lax.all_gather(outer_gate_weight, "sp", axis=0, tiled=True),
            lax.all_gather(inner_gate_weight, "sp", axis=0, tiled=True),
            lax.all_gather(signal_weight, "sp", axis=0, tiled=True),
        ),
        jnp.int32(0),
    )
    mixer = mixer_local(normed, (query, keyed, valued), *mixer_args)
    (query_per_head, key_per_head, value_per_head), recalled, probe, final_state, final_product = (
        mixer
    )
    number_heads, head_dimension = (query_per_head.shape[1], query_per_head.shape[2])
    position = lax.axis_index("sp")

    def hand_on(turn, entering_now):
        outgoing = contract("hvk,hkj->hvj", entering_now, final_product) + final_state
        moved = from_behind(outgoing.astype(jnp.bfloat16), "sp", 1).astype(outgoing.dtype)
        return jnp.where(position == 0, starting_state, moved)

    entering = lax.fori_loop(0, lax.axis_size("sp") - 1, hand_on, starting_state)
    recalled = recalled + contract("hvk,thk->thv", entering, probe)
    center = recalled - jnp.mean(recalled, axis=2, keepdims=True)
    variance = jnp.mean(center * center, axis=2, keepdims=True)
    input_normed = (
        center
        * lax.rsqrt(variance + GROUP_EPS)
        * head_norm_gain.reshape(number_heads, head_dimension)
    )
    own_term = (
        jnp.sum(
            query_per_head * key_per_head * own_term_weight.reshape(number_heads, head_dimension),
            axis=2,
            keepdims=True,
        )
        * value_per_head
    )
    linear_attention_output = (
        (input_normed + own_term)
        .reshape(sequence_length, number_heads * head_dimension)
        .astype(jnp.bfloat16)
    )
    outer_f = rounded(outer)
    mixed_in = (rounded(inner) * rounded(signal)).astype(jnp.bfloat16)
    previous = from_behind(mixed_in[sequence_length - 2 :], "sp", 1)
    padded = jnp.concatenate([previous, mixed_in], axis=0).astype(jnp.float32)
    taps = convolution_taps.astype(jnp.float32)
    gated = outer_f * (taps[0] * padded[:-2] + taps[1] * padded[1:-1] + taps[2] * padded[2:])
    squares = lax.psum(jnp.sum(gated * gated, axis=1), "tp")
    channel_total = gated.shape[1] * lax.axis_size("tp")
    out_conv = (
        gated * lax.rsqrt(squares[:, None] / channel_total + NORM_EPS) * convolution_gain
    ).astype(jnp.bfloat16)
    return (linear_attention_output, out_conv)


HEAD_ROWS = 8


def head_kernel(
    x_ref, w_ref, pos_ref, extra_ref, decay_map_ref, rate_map_ref, chan_ref, start_ref,
    lin_ref, gated_ref, state_ref, conv_ref,
):
    f32, bf16 = jnp.float32, jnp.bfloat16
    spans, pieces, rows, depth = x_ref.shape
    positions = spans * rows
    size = start_ref.shape[0]
    count = positions // BLOCK

    @pl.when(pl.program_id(0) == 0)
    def _():
        state_ref[...] = start_ref[...]
        conv_ref[pl.ds(0, HEAD_ROWS), :] = jnp.zeros((HEAD_ROWS, size), f32)

    @pl.when(pl.program_id(0) > 0)
    def _():
        conv_ref[pl.ds(0, HEAD_ROWS), :] = conv_ref[pl.ds(positions, HEAD_ROWS), :]

    def exact(left, right, dims=((1,), (0,))):
        return lax.dot_general(
            left, right, (dims, ((), ())),
            precision=lax.Precision.HIGHEST, preferred_element_type=f32,
        )

    def held(values):
        return values.astype(bf16).astype(f32)

    proj = None
    for piece in range(pieces):
        left = x_ref[:, piece].reshape(positions, depth)
        term = jnp.dot(left, w_ref[piece], preferred_element_type=f32)
        proj = term if proj is None else proj + term

    def halves(index):
        slab = proj[:, index * 2 * size : (index + 1) * 2 * size]
        return held(slab[:, :size]), held(pltpu.roll(slab, size, 1)[:, :size])

    query, keyed = halves(0)
    valued, outer = halves(1)
    inner, signal = halves(2)
    rank = decay_map_ref.shape[0]
    decay_low = jnp.tanh(proj[:, 6 * size : 6 * size + rank]).astype(bf16)
    rate_low = proj[:, 6 * size + rank : 6 * size + 2 * rank].astype(bf16)
    chan = chan_ref[...]
    logits = (
        chan[0:1]
        + jnp.dot(decay_low, decay_map_ref[...], preferred_element_type=f32)
        + pos_ref[...]
    )
    log_decay = -DECAY_FACTOR * jax.nn.sigmoid(logits) + extra_ref[...]
    rate = jax.nn.sigmoid(
        chan[1:2] + jnp.dot(rate_low, rate_map_ref[...], preferred_element_type=f32)
    )
    unit = keyed * lax.rsqrt(jnp.sum(keyed * keyed, axis=1, keepdims=True) + KEY_EPS)

    mixed = held(inner * signal)
    conv_ref[pl.ds(HEAD_ROWS, positions), :] = mixed
    gated_ref[...] = outer * (
        chan[4:5] * conv_ref[pl.ds(HEAD_ROWS - 2, positions), :]
        + chan[5:6] * conv_ref[pl.ds(HEAD_ROWS - 1, positions), :]
        + chan[6:7] * mixed
    )

    later = lax.broadcasted_iota(jnp.int32, (BLOCK, BLOCK), 0)
    earlier = lax.broadcasted_iota(jnp.int32, (BLOCK, BLOCK), 1)
    strict, inclusive = later > earlier, later >= earlier
    eye = (later == earlier).astype(f32)
    tri = inclusive.astype(f32)
    every = range(count)

    def cut(values):
        return [values[g * BLOCK : (g + 1) * BLOCK] for g in every]

    q, k, v, u, d = cut(query), cut(keyed), cut(valued), cut(unit), cut(log_decay)
    ur = cut(unit * rate)
    total = [exact(tri, d[g]) for g in every]
    before = [total[g] - d[g] for g in every]
    middle = [total[g][BLOCK // 2 - 1 : BLOCK // 2] for g in every]
    closing = [total[g][BLOCK - 1 : BLOCK] for g in every]
    fall = [jnp.exp(middle[g] - total[g]) for g in every]
    left = [
        jnp.concatenate(
            [-u[g] * jnp.exp(before[g] - middle[g]), q[g] * jnp.exp(total[g] - middle[g])], axis=0
        )
        for g in every
    ]
    over_b = [exact(left[g], ur[g] * fall[g], ((1,), (1,))) for g in every]
    over_k = [exact(left[g], k[g] * fall[g], ((1,), (1,))) for g in every]
    removal = [jnp.where(strict, over_b[g][:BLOCK], 0.0) for g in every]
    reads = [jnp.where(inclusive, over_b[g][BLOCK:], 0.0) for g in every]
    on_values = [
        exact(
            jnp.concatenate(
                [
                    jnp.where(strict, over_k[g][:BLOCK], 0.0),
                    jnp.where(inclusive, over_k[g][BLOCK:], 0.0),
                ],
                axis=0,
            ),
            v[g],
        )
        for g in every
    ]
    inverse = [eye + removal[g] for g in every]
    power = [exact(removal[g], removal[g]) for g in every]
    reach = 4
    while reach < BLOCK:
        both = [
            exact(jnp.concatenate([inverse[g], power[g]], axis=0), power[g]) for g in every
        ]
        inverse = [inverse[g] + both[g][:BLOCK] for g in every]
        power = [both[g][BLOCK:] for g in every]
        reach = reach * 2
    inverse = [inverse[g] + exact(inverse[g], power[g]) for g in every]
    unit_solved = [exact(inverse[g], -u[g] * jnp.exp(before[g])) for g in every]
    free_solved = [exact(inverse[g], on_values[g][:BLOCK]) for g in every]
    probe = [q[g] * jnp.exp(total[g]) + exact(reads[g], unit_solved[g]) for g in every]
    free_read = [exact(reads[g], free_solved[g]) + on_values[g][BLOCK:] for g in every]
    rest = [jnp.exp(closing[g] - total[g]) for g in every]
    b_end = [ur[g] * rest[g] for g in every]
    k_end = [k[g] * rest[g] for g in every]
    first = ((0,), (0,))
    step = [
        eye * jnp.exp(closing[g]) + exact(unit_solved[g], b_end[g], first) for g in every
    ]
    added = [
        exact(free_solved[g], b_end[g], first) + exact(v[g], k_end[g], first) for g in every
    ]
    state = state_ref[...]
    entering = []
    for g in every:
        entering.append(state)
        state = exact(state, step[g]) + added[g]
    state_ref[...] = state
    recalled = jnp.concatenate(
        [exact(probe[g], entering[g], ((1,), (1,))) + free_read[g] for g in every], axis=0
    )
    center = recalled - jnp.mean(recalled, axis=1, keepdims=True)
    variance = jnp.mean(center * center, axis=1, keepdims=True)
    own = jnp.sum(query * keyed * chan[2:3], axis=1, keepdims=True) * valued
    lin_ref[...] = (center * lax.rsqrt(variance + GROUP_EPS) * chan[3:4] + own).astype(bf16)


def run_head(gathered, weights, pos, extra, decay_map, rate_map, chan, start):
    spans, pieces, rows, depth = gathered.shape
    group = 2 if spans % 2 == 0 else 1
    positions, size, rank = group * rows, start.shape[0], decay_map.shape[0]
    length = spans * rows
    width = weights.shape[2]

    def fixed(shape):
        return pl.BlockSpec(shape, lambda i: (0,) * len(shape))

    def along(columns):
        return pl.BlockSpec((positions, columns), lambda i: (i, 0))

    return pl.pallas_call(
        head_kernel,
        grid=(spans // group,),
        out_shape=(
            jax.ShapeDtypeStruct((length, size), jnp.bfloat16),
            jax.ShapeDtypeStruct((length, size), jnp.float32),
        ),
        in_specs=[
            pl.BlockSpec((group, pieces, rows, depth), lambda i: (i, 0, 0, 0)),
            fixed((pieces, depth, width)),
            along(1),
            along(1),
            fixed((rank, size)),
            fixed((rank, size)),
            fixed(chan.shape),
            fixed((size, size)),
        ],
        out_specs=(along(size), along(size)),
        scratch_shapes=[
            pltpu.VMEM((size, size), jnp.float32),
            pltpu.VMEM((positions + HEAD_ROWS, size), jnp.float32),
        ],
        compiler_params=pltpu.CompilerParams(vmem_limit_bytes=56 * 1024 * 1024),
        cost_estimate=pl.CostEstimate(
            flops=2 * length * pieces * depth * width,
            bytes_accessed=2 * length * pieces * depth,
            transcendentals=0,
        ),
        name="head",
    )(gathered, weights, pos, extra, decay_map, rate_map, chan, start)


def per_head(
    tokens,
    input_norm_gain,
    query_weight,
    key_weight,
    value_weight,
    decay_first_map,
    decay_second_map,
    channel_decay_offset,
    position_decay_offset,
    extra_log_decay,
    rate_first_map,
    rate_second_map,
    channel_rate_offset,
    own_term_weight,
    head_norm_gain,
    starting_state,
    outer_gate_weight,
    inner_gate_weight,
    signal_weight,
    convolution_taps,
    convolution_gain,
):
    devices, splits = lax.axis_size("sp"), lax.axis_size("tp")
    mine, column = lax.axis_index("sp"), lax.axis_index("tp")
    rows, depth = tokens.shape
    features = depth * splits
    size = starting_state.shape[2]
    weights = jnp.stack(
        [query_weight, key_weight, value_weight, outer_gate_weight, inner_gate_weight, signal_weight]
    )
    deep = query_weight.shape[0]
    parcels = jnp.transpose(
        weights.reshape(6, deep, devices, size), (2, 1, 0, 3)
    ).reshape(devices, deep, 6 * size)
    wide = tokens.astype(jnp.float32)
    squares = lax.psum(jnp.sum(wide * wide, axis=1), "tp")
    gain = lax.dynamic_slice(input_norm_gain, (column * depth,), (depth,))
    normed = (wide * lax.rsqrt(squares[:, None] / features + NORM_EPS) * gain).astype(jnp.bfloat16)
    moved = lax.all_to_all(parcels, "sp", 0, 0, tiled=True)
    gathered = lax.all_gather(normed, ("sp", "tp"), axis=0, tiled=False)
    small = lax.all_gather(
        jnp.concatenate([position_decay_offset[:, None], extra_log_decay], axis=1),
        "sp", axis=0, tiled=True,
    )
    pos = small[:, :1]
    extra = lax.dynamic_slice(small, (0, 1 + mine), (small.shape[0], 1))
    whole_weights = jnp.concatenate(
        [moved.reshape(features, 6 * size), decay_first_map, rate_first_map], axis=1
    ).reshape(splits, depth, -1)

    def own(values):
        return lax.dynamic_slice_in_dim(values, mine * size, size, axis=values.ndim - 1)

    chan = jnp.stack(
        [
            own(channel_decay_offset),
            own(channel_rate_offset),
            own(own_term_weight),
            own(head_norm_gain),
            *own(convolution_taps).astype(jnp.float32),
            own(convolution_gain),
        ]
    )
    start = lax.dynamic_index_in_dim(starting_state, mine, 0, keepdims=False)
    linear, gated = run_head(
        gathered.reshape(devices, splits, rows, depth),
        whole_weights, pos, extra, own(decay_second_map), own(rate_second_map), chan, start,
    )
    sums = lax.psum(jnp.sum(gated * gated, axis=1), ("sp", "tp"))
    channels = size * devices * splits
    conv = (gated * lax.rsqrt(sums[:, None] / channels + NORM_EPS) * chan[7]).astype(jnp.bfloat16)
    back = lax.all_to_all(
        jnp.concatenate([linear, conv], axis=1).reshape(devices, rows, 2 * size),
        "sp", 0, 0, tiled=True,
    )
    back = jnp.transpose(back.reshape(devices, rows, 2, size), (2, 1, 0, 3))
    back = back.reshape(2, rows, devices * size)
    return (back[0], back[1])


def plan(*arrays):
    heads = arrays[15].shape[0]
    if heads == lax.axis_size("sp") and arrays[0].shape[0] % BLOCK == 0:
        return per_head(*arrays)
    return shards(*arrays)


def solution(mesh):
    placed = (
        P("sp", "tp"),
        P(),
        P("sp", "tp"),
        P("sp", "tp"),
        P("sp", "tp"),
        P(),
        P(None, "tp"),
        P("tp"),
        P("sp"),
        P("sp", "tp"),
        P(),
        P(None, "tp"),
        P("tp"),
        P("tp"),
        P("tp"),
        P("tp", None, None),
        P("sp", "tp"),
        P("sp", "tp"),
        P("sp", "tp"),
        P(None, "tp"),
        P("tp"),
    )
    return jax.shard_map(
        plan,
        mesh=mesh,
        in_specs=placed,
        out_specs=(P("sp", "tp"), P("sp", "tp")),
        check_vma=False,
    )
```

```python
import functools

import jax
import jax.numpy as jnp
from jax import lax
from jax.experimental import pallas as pl
from jax.experimental.pallas import tpu as pltpu
from jax.sharding import PartitionSpec as P

BLOCK = 64


DECAY_FACTOR = 0.606531
NORM_EPS = 1e-06
GROUP_EPS = 0.00064
KEY_EPS = 1e-06


def from_behind(block, axis, distance):
    devices = range(lax.axis_size(axis))
    route = [(i - distance, i) for i in devices if i - distance in devices]
    return lax.ppermute(block, axis, route)


def rounded(values):
    return lax.optimization_barrier(values.astype(jnp.bfloat16)).astype(jnp.float32)


def contract(spec, left, right):
    return jnp.einsum(spec, left, right, precision=lax.Precision.HIGHEST)


def fold_rows(normed):

    def accumulate(totals, pieces, offset):
        return tuple(
            (
                jnp.dot(normed, weight_piece, preferred_element_type=jnp.float32)
                for weight_piece in pieces
            )
        )

    return accumulate


def mixer_blocks(query, keyed, valued, unit_key, decay_logarithm, rate):
    sequence_length, number_heads, head_dimension = query.shape
    block_size = BLOCK
    count = sequence_length // block_size
    eye_heads = jnp.broadcast_to(
        jnp.eye(head_dimension, dtype=jnp.float32), (number_heads, head_dimension, head_dimension)
    )
    eye_block = jnp.eye(block_size, dtype=jnp.float32)
    later = jnp.arange(block_size)[:, None]
    earlier = jnp.arange(block_size)[None, :]
    strict = later > earlier
    inclusive = later >= earlier
    block_shape = (count, block_size, number_heads, head_dimension)
    query_b, keyed_b, valued_b, unit_b, decay_b, rate_b = (
        values.reshape(block_shape)
        for values in (query, keyed, valued, unit_key, decay_logarithm, rate)
    )
    cumul = jnp.cumsum(decay_b, axis=1)
    before = cumul - decay_b
    a_prime = -unit_b * jnp.exp(before)
    b_scaled = unit_b * rate_b * jnp.exp(-cumul)
    k_scaled = keyed_b * jnp.exp(-cumul)
    r_prime = query_b * jnp.exp(cumul)
    removal = jnp.where(strict, contract("cthn,cshn->chts", a_prime, b_scaled), 0.0)
    writes = jnp.where(strict, contract("cthn,cshn->chts", a_prime, k_scaled), 0.0)
    reads = jnp.where(inclusive, contract("cthn,cshn->chts", r_prime, b_scaled), 0.0)
    key_reads = jnp.where(inclusive, contract("cthn,cshn->chts", r_prime, k_scaled), 0.0)
    power = removal
    inverse = eye_block + removal
    reach = 2
    while reach < block_size:
        power = contract("chts,chsu->chtu", power, power)
        inverse = inverse + contract("chts,chsu->chtu", inverse, power)
        reach = reach * 2
    unit_solved = contract("chts,cshn->chtn", inverse, a_prime)
    free_solved = contract(
        "chts,chsv->chtv", inverse, contract("chts,cshv->chtv", writes, valued_b)
    )
    probe_raw = jnp.transpose(r_prime, (0, 2, 1, 3)) + contract(
        "chts,chsn->chtn", reads, unit_solved
    )
    free_read = contract("chts,chsv->chtv", reads, free_solved) + contract(
        "chts,cshv->chtv", key_reads, valued_b
    )
    closing = jnp.exp(cumul[:, -1])
    b_end = b_scaled * closing[:, None]
    k_end = k_scaled * closing[:, None]
    step_map = eye_heads[None] * closing[:, :, None, :] + contract(
        "chtj,cthk->chjk", unit_solved, b_end
    )
    constant = contract("chtv,cthk->chvk", free_solved, b_end) + contract(
        "cthv,cthk->chvk", valued_b, k_end
    )
    local_state = jnp.zeros((number_heads, head_dimension, head_dimension), jnp.float32)
    product = eye_heads
    entering_states = []
    entering_maps = []
    for index in range(count):
        entering_states.append(local_state)
        entering_maps.append(product)
        local_state = contract("hvk,hkj->hvj", local_state, step_map[index]) + constant[index]
        product = contract("hij,hjk->hik", product, step_map[index])
    stacked_states = jnp.stack(entering_states)
    stacked_maps = jnp.stack(entering_maps)
    recalled = contract("chvk,chtk->cthv", stacked_states, probe_raw) + jnp.transpose(
        free_read, (0, 2, 1, 3)
    )
    probe = contract("chjk,chtk->cthj", stacked_maps, probe_raw)
    head_shape = (sequence_length, number_heads, head_dimension)
    return (recalled.reshape(head_shape), probe.reshape(head_shape), local_state, product)


def mixer_local(
    normed,
    projected,
    decay_first_map,
    decay_second_map,
    channel_decay_offset,
    position_decay_offset,
    extra_log_decay,
    rate_first_map,
    rate_second_map,
    channel_rate_offset,
):
    query, keyed, valued = (rounded(values) for values in projected)
    sequence_length = normed.shape[0]
    number_heads = extra_log_decay.shape[1]
    head_dimension = query.shape[1] // number_heads
    decay_low = jnp.tanh(
        jnp.dot(normed, decay_first_map, preferred_element_type=jnp.float32)
    ).astype(jnp.bfloat16)
    decay_logits = (
        channel_decay_offset
        + jnp.dot(decay_low, decay_second_map, preferred_element_type=jnp.float32)
        + position_decay_offset[:, None]
    )
    decay_logarithm = -DECAY_FACTOR * jax.nn.sigmoid(decay_logits) + jnp.repeat(
        extra_log_decay, head_dimension, axis=1
    )
    rate_low = jnp.dot(normed, rate_first_map, preferred_element_type=jnp.float32).astype(
        jnp.bfloat16
    )
    rate = jax.nn.sigmoid(
        channel_rate_offset + jnp.dot(rate_low, rate_second_map, preferred_element_type=jnp.float32)
    )
    head_shape = (sequence_length, number_heads, head_dimension)
    query_per_head = query.reshape(head_shape)
    key_per_head = keyed.reshape(head_shape)
    value_per_head = valued.reshape(head_shape)
    unit_key = key_per_head * lax.rsqrt(
        jnp.sum(key_per_head * key_per_head, axis=2, keepdims=True) + KEY_EPS
    )
    recalled, probe, final_state, final_product = mixer_blocks(
        query_per_head,
        key_per_head,
        value_per_head,
        unit_key,
        decay_logarithm.reshape(head_shape),
        rate.reshape(head_shape),
    )
    return (
        (query_per_head, key_per_head, value_per_head),
        recalled,
        probe,
        final_state,
        final_product,
    )


def shards(
    tokens,
    input_norm_gain,
    query_weight,
    key_weight,
    value_weight,
    decay_first_map,
    decay_second_map,
    channel_decay_offset,
    position_decay_offset,
    extra_log_decay,
    rate_first_map,
    rate_second_map,
    channel_rate_offset,
    own_term_weight,
    head_norm_gain,
    starting_state,
    outer_gate_weight,
    inner_gate_weight,
    signal_weight,
    convolution_taps,
    convolution_gain,
):
    whole = lax.all_gather(tokens, "tp", axis=1, tiled=True)
    wide = whole.astype(jnp.float32)
    normed = (
        wide * lax.rsqrt(jnp.mean(wide * wide, axis=1, keepdims=True) + NORM_EPS) * input_norm_gain
    ).astype(jnp.bfloat16)
    sequence_length = normed.shape[0]
    accumulate = fold_rows(normed)
    empty = jnp.zeros((sequence_length, query_weight.shape[1]), jnp.float32)
    mixer_args = (
        decay_first_map,
        decay_second_map,
        channel_decay_offset,
        position_decay_offset,
        extra_log_decay,
        rate_first_map,
        rate_second_map,
        channel_rate_offset,
    )
    query, keyed, valued, outer, inner, signal = accumulate(
        (empty, empty, empty, empty, empty, empty),
        (
            lax.all_gather(query_weight, "sp", axis=0, tiled=True),
            lax.all_gather(key_weight, "sp", axis=0, tiled=True),
            lax.all_gather(value_weight, "sp", axis=0, tiled=True),
            lax.all_gather(outer_gate_weight, "sp", axis=0, tiled=True),
            lax.all_gather(inner_gate_weight, "sp", axis=0, tiled=True),
            lax.all_gather(signal_weight, "sp", axis=0, tiled=True),
        ),
        jnp.int32(0),
    )
    mixer = mixer_local(normed, (query, keyed, valued), *mixer_args)
    (query_per_head, key_per_head, value_per_head), recalled, probe, final_state, final_product = (
        mixer
    )
    number_heads, head_dimension = (query_per_head.shape[1], query_per_head.shape[2])
    position = lax.axis_index("sp")

    def hand_on(turn, entering_now):
        outgoing = contract("hvk,hkj->hvj", entering_now, final_product) + final_state
        moved = from_behind(outgoing.astype(jnp.bfloat16), "sp", 1).astype(outgoing.dtype)
        return jnp.where(position == 0, starting_state, moved)

    entering = lax.fori_loop(0, lax.axis_size("sp") - 1, hand_on, starting_state)
    recalled = recalled + contract("hvk,thk->thv", entering, probe)
    center = recalled - jnp.mean(recalled, axis=2, keepdims=True)
    variance = jnp.mean(center * center, axis=2, keepdims=True)
    input_normed = (
        center
        * lax.rsqrt(variance + GROUP_EPS)
        * head_norm_gain.reshape(number_heads, head_dimension)
    )
    own_term = (
        jnp.sum(
            query_per_head * key_per_head * own_term_weight.reshape(number_heads, head_dimension),
            axis=2,
            keepdims=True,
        )
        * value_per_head
    )
    linear_attention_output = (
        (input_normed + own_term)
        .reshape(sequence_length, number_heads * head_dimension)
        .astype(jnp.bfloat16)
    )
    outer_f = rounded(outer)
    mixed_in = (rounded(inner) * rounded(signal)).astype(jnp.bfloat16)
    previous = from_behind(mixed_in[sequence_length - 2 :], "sp", 1)
    padded = jnp.concatenate([previous, mixed_in], axis=0).astype(jnp.float32)
    taps = convolution_taps.astype(jnp.float32)
    gated = outer_f * (taps[0] * padded[:-2] + taps[1] * padded[1:-1] + taps[2] * padded[2:])
    squares = lax.psum(jnp.sum(gated * gated, axis=1), "tp")
    channel_total = gated.shape[1] * lax.axis_size("tp")
    out_conv = (
        gated * lax.rsqrt(squares[:, None] / channel_total + NORM_EPS) * convolution_gain
    ).astype(jnp.bfloat16)
    return (linear_attention_output, out_conv)


HEAD_ROWS = 8


def head_kernel(
    x_ref, w_ref, pos_ref, extra_ref, decay_map_ref, rate_map_ref, chan_ref, start_ref,
    lin_ref, gated_ref, state_ref, conv_ref,
):
    f32, bf16 = jnp.float32, jnp.bfloat16
    spans, pieces, rows, depth = x_ref.shape
    positions = spans * rows
    size = start_ref.shape[0]
    count = positions // BLOCK

    @pl.when(pl.program_id(0) == 0)
    def _():
        state_ref[...] = start_ref[...]
        conv_ref[pl.ds(0, HEAD_ROWS), :] = jnp.zeros((HEAD_ROWS, size), f32)

    @pl.when(pl.program_id(0) > 0)
    def _():
        conv_ref[pl.ds(0, HEAD_ROWS), :] = conv_ref[pl.ds(positions, HEAD_ROWS), :]

    def once(left, right, dims):
        return lax.dot_general(left, right, (dims, ((), ())), preferred_element_type=f32)

    def exact(left, right, dims=((1,), (0,))):
        left_high, right_high = left.astype(bf16), right.astype(bf16)
        left_low = (left - left_high.astype(f32)).astype(bf16)
        right_low = (right - right_high.astype(f32)).astype(bf16)
        return once(left_high, right_high, dims) + (
            once(left_high, right_low, dims) + once(left_low, right_high, dims)
        )

    def held(values):
        return values.astype(bf16).astype(f32)

    proj = None
    for piece in range(pieces):
        left = x_ref[:, piece].reshape(positions, depth)
        term = jnp.dot(left, w_ref[piece], preferred_element_type=f32)
        proj = term if proj is None else proj + term

    def halves(index):
        slab = proj[:, index * 2 * size : (index + 1) * 2 * size]
        return held(slab[:, :size]), held(pltpu.roll(slab, size, 1)[:, :size])

    query, keyed = halves(0)
    valued, outer = halves(1)
    inner, signal = halves(2)
    rank = decay_map_ref.shape[0]
    decay_low = jnp.tanh(proj[:, 6 * size : 6 * size + rank]).astype(bf16)
    rate_low = proj[:, 6 * size + rank : 6 * size + 2 * rank].astype(bf16)
    chan = chan_ref[...]
    logits = (
        chan[0:1]
        + jnp.dot(decay_low, decay_map_ref[...], preferred_element_type=f32)
        + pos_ref[...]
    )
    log_decay = -DECAY_FACTOR * jax.nn.sigmoid(logits) + extra_ref[...]
    rate = jax.nn.sigmoid(
        chan[1:2] + jnp.dot(rate_low, rate_map_ref[...], preferred_element_type=f32)
    )
    unit = keyed * lax.rsqrt(jnp.sum(keyed * keyed, axis=1, keepdims=True) + KEY_EPS)

    mixed = held(inner * signal)
    conv_ref[pl.ds(HEAD_ROWS, positions), :] = mixed
    gated = outer * (
        chan[4:5] * conv_ref[pl.ds(HEAD_ROWS - 2, positions), :]
        + chan[5:6] * conv_ref[pl.ds(HEAD_ROWS - 1, positions), :]
        + chan[6:7] * mixed
    )
    gated_ref[...] = gated.astype(bf16)

    later = lax.broadcasted_iota(jnp.int32, (BLOCK, BLOCK), 0)
    earlier = lax.broadcasted_iota(jnp.int32, (BLOCK, BLOCK), 1)
    strict, inclusive = later > earlier, later >= earlier
    eye = (later == earlier).astype(f32)
    tri = inclusive.astype(f32)
    every = range(count)

    def cut(values):
        return [values[g * BLOCK : (g + 1) * BLOCK] for g in every]

    q, k, v, u, d = cut(query), cut(keyed), cut(valued), cut(unit), cut(log_decay)
    ur = cut(unit * rate)
    total = [
        jnp.dot(tri, d[g], precision=lax.Precision.HIGHEST, preferred_element_type=f32)
        for g in every
    ]
    before = [total[g] - d[g] for g in every]
    middle = [total[g][BLOCK // 2 - 1 : BLOCK // 2] for g in every]
    closing = [total[g][BLOCK - 1 : BLOCK] for g in every]
    fall = [jnp.exp(middle[g] - total[g]) for g in every]
    left = [
        jnp.concatenate(
            [-u[g] * jnp.exp(before[g] - middle[g]), q[g] * jnp.exp(total[g] - middle[g])], axis=0
        )
        for g in every
    ]
    over_b = [exact(left[g], ur[g] * fall[g], ((1,), (1,))) for g in every]
    over_k = [exact(left[g], k[g] * fall[g], ((1,), (1,))) for g in every]
    removal = [jnp.where(strict, over_b[g][:BLOCK], 0.0) for g in every]
    reads = [jnp.where(inclusive, over_b[g][BLOCK:], 0.0) for g in every]
    on_values = [
        exact(
            jnp.concatenate(
                [
                    jnp.where(strict, over_k[g][:BLOCK], 0.0),
                    jnp.where(inclusive, over_k[g][BLOCK:], 0.0),
                ],
                axis=0,
            ),
            v[g],
        )
        for g in every
    ]
    inverse = [eye + removal[g] for g in every]
    power = [exact(removal[g], removal[g]) for g in every]
    reach = 4
    while reach < BLOCK:
        both = [
            exact(jnp.concatenate([inverse[g], power[g]], axis=0), power[g]) for g in every
        ]
        inverse = [inverse[g] + both[g][:BLOCK] for g in every]
        power = [both[g][BLOCK:] for g in every]
        reach = reach * 2
    inverse = [inverse[g] + exact(inverse[g], power[g]) for g in every]
    unit_solved = [exact(inverse[g], -u[g] * jnp.exp(before[g])) for g in every]
    free_solved = [exact(inverse[g], on_values[g][:BLOCK]) for g in every]
    probe = [q[g] * jnp.exp(total[g]) + exact(reads[g], unit_solved[g]) for g in every]
    free_read = [exact(reads[g], free_solved[g]) + on_values[g][BLOCK:] for g in every]
    rest = [jnp.exp(closing[g] - total[g]) for g in every]
    b_end = [ur[g] * rest[g] for g in every]
    k_end = [k[g] * rest[g] for g in every]
    first = ((0,), (0,))
    step = [
        eye * jnp.exp(closing[g]) + exact(unit_solved[g], b_end[g], first) for g in every
    ]
    added = [
        exact(free_solved[g], b_end[g], first) + exact(v[g], k_end[g], first) for g in every
    ]
    state = state_ref[...]
    entering = []
    for g in every:
        entering.append(state)
        state = exact(state, step[g]) + added[g]
    state_ref[...] = state
    recalled = jnp.concatenate(
        [exact(probe[g], entering[g], ((1,), (1,))) + free_read[g] for g in every], axis=0
    )
    center = recalled - jnp.mean(recalled, axis=1, keepdims=True)
    variance = jnp.mean(center * center, axis=1, keepdims=True)
    own = jnp.sum(query * keyed * chan[2:3], axis=1, keepdims=True) * valued
    lin_ref[...] = (center * lax.rsqrt(variance + GROUP_EPS) * chan[3:4] + own).astype(bf16)


def run_head(gathered, weights, pos, extra, decay_map, rate_map, chan, start):
    spans, pieces, rows, depth = gathered.shape
    group = 1
    positions, size, rank = group * rows, start.shape[0], decay_map.shape[0]
    length = spans * rows
    width = weights.shape[2]

    def fixed(shape):
        return pl.BlockSpec(shape, lambda i: (0,) * len(shape))

    def along(columns):
        return pl.BlockSpec((positions, columns), lambda i: (i, 0))

    return pl.pallas_call(
        head_kernel,
        grid=(spans // group,),
        out_shape=(
            jax.ShapeDtypeStruct((length, size), jnp.bfloat16),
            jax.ShapeDtypeStruct((length, size), jnp.bfloat16),
        ),
        in_specs=[
            pl.BlockSpec((group, pieces, rows, depth), lambda i: (i, 0, 0, 0)),
            fixed((pieces, depth, width)),
            along(1),
            along(1),
            fixed((rank, size)),
            fixed((rank, size)),
            fixed(chan.shape),
            fixed((size, size)),
        ],
        out_specs=(along(size), along(size)),
        scratch_shapes=[
            pltpu.VMEM((size, size), jnp.float32),
            pltpu.VMEM((positions + HEAD_ROWS, size), jnp.float32),
        ],
        compiler_params=pltpu.CompilerParams(vmem_limit_bytes=56 * 1024 * 1024),
        cost_estimate=pl.CostEstimate(
            flops=2 * length * pieces * depth * width,
            bytes_accessed=2 * length * pieces * depth,
            transcendentals=0,
        ),
        name="head",
    )(gathered, weights, pos, extra, decay_map, rate_map, chan, start)


def per_head(
    tokens,
    input_norm_gain,
    query_weight,
    key_weight,
    value_weight,
    decay_first_map,
    decay_second_map,
    channel_decay_offset,
    position_decay_offset,
    extra_log_decay,
    rate_first_map,
    rate_second_map,
    channel_rate_offset,
    own_term_weight,
    head_norm_gain,
    starting_state,
    outer_gate_weight,
    inner_gate_weight,
    signal_weight,
    convolution_taps,
    convolution_gain,
):
    devices, splits = lax.axis_size("sp"), lax.axis_size("tp")
    mine, column = lax.axis_index("sp"), lax.axis_index("tp")
    rows, depth = tokens.shape
    features = depth * splits
    size = starting_state.shape[2]
    weights = jnp.stack(
        [query_weight, key_weight, value_weight, outer_gate_weight, inner_gate_weight, signal_weight]
    )
    deep = query_weight.shape[0]
    parcels = jnp.transpose(
        weights.reshape(6, deep, devices, size), (2, 1, 0, 3)
    ).reshape(devices, deep, 6 * size)
    wide = tokens.astype(jnp.float32)
    squares = lax.psum(jnp.sum(wide * wide, axis=1), "tp")
    gain = lax.dynamic_slice(input_norm_gain, (column * depth,), (depth,))
    normed = (wide * lax.rsqrt(squares[:, None] / features + NORM_EPS) * gain).astype(jnp.bfloat16)
    moved = lax.all_to_all(parcels, "sp", 0, 0, tiled=True)
    gathered = lax.all_gather(normed, ("sp", "tp"), axis=0, tiled=False)
    small = lax.all_gather(
        jnp.concatenate([position_decay_offset[:, None], extra_log_decay], axis=1),
        "sp", axis=0, tiled=True,
    )
    pos = small[:, :1]
    extra = lax.dynamic_slice(small, (0, 1 + mine), (small.shape[0], 1))
    whole_weights = jnp.concatenate(
        [moved.reshape(features, 6 * size), decay_first_map, rate_first_map], axis=1
    ).reshape(splits, depth, -1)

    def own(values):
        return lax.dynamic_slice_in_dim(values, mine * size, size, axis=values.ndim - 1)

    chan = jnp.stack(
        [
            own(channel_decay_offset),
            own(channel_rate_offset),
            own(own_term_weight),
            own(head_norm_gain),
            *own(convolution_taps).astype(jnp.float32),
            jnp.zeros((size,), jnp.float32),
        ]
    )
    start = lax.dynamic_index_in_dim(starting_state, mine, 0, keepdims=False)
    linear, gated = run_head(
        gathered.reshape(devices, splits, rows, depth),
        whole_weights, pos, extra, own(decay_second_map), own(rate_second_map), chan, start,
    )
    back = lax.all_to_all(
        jnp.concatenate([linear, gated], axis=1).reshape(devices, rows, 2 * size),
        "sp", 0, 0, tiled=True,
    )
    back = jnp.transpose(back.reshape(devices, rows, 2, size), (2, 1, 0, 3))
    back = back.reshape(2, rows, devices * size)
    gated = back[1].astype(jnp.float32)
    sums = lax.psum(jnp.sum(gated * gated, axis=1), "tp")
    channels = size * devices * splits
    conv = gated * lax.rsqrt(sums[:, None] / channels + NORM_EPS) * convolution_gain
    return (back[0], conv.astype(jnp.bfloat16))


def plan(*arrays):
    heads = arrays[15].shape[0]
    if heads == lax.axis_size("sp") and arrays[0].shape[0] % BLOCK == 0:
        return per_head(*arrays)
    return shards(*arrays)


def solution(mesh):
    placed = (
        P("sp", "tp"),
        P(),
        P("sp", "tp"),
        P("sp", "tp"),
        P("sp", "tp"),
        P(),
        P(None, "tp"),
        P("tp"),
        P("sp"),
        P("sp", "tp"),
        P(),
        P(None, "tp"),
        P("tp"),
        P("tp"),
        P("tp"),
        P("tp", None, None),
        P("sp", "tp"),
        P("sp", "tp"),
        P("sp", "tp"),
        P(None, "tp"),
        P("tp"),
    )
    return jax.shard_map(
        plan,
        mesh=mesh,
        in_specs=placed,
        out_specs=(P("sp", "tp"), P("sp", "tp")),
        check_vma=False,
    )
```
